32 devices in a mesh: sp: 16 (over z, y, core), tp: 2 (over x).
Axes of the slice: x: 2, y: 2, z: 4, core: 2. Of those that a mesh axis runs over, the one named last changes fastest.
Arguments:
- tokens_in: bfloat16 [4096, 2048], P('sp', 'tp'), may hold values from -400 to 400
- norm_gain: float32 [2048], replicated, may hold values from 0.1 to 1.9
- w_query: bfloat16 [2048, 1024], P('sp', 'tp'), may hold values from -0.125 to 0.125
- w_forget: bfloat16 [2048, 1024], P('sp', 'tp'), may hold values from -0.125 to 0.125
- w_input: bfloat16 [2048, 1024], P('sp', 'tp'), may hold values from -0.125 to 0.125
- w_rgate: bfloat16 [2048, 1024], P('sp', 'tp'), may hold values from -0.125 to 0.125
- w_pool_in: bfloat16 [2048, 1024], P('sp', 'tp'), may hold values from -0.125 to 0.125
- w_pgate: bfloat16 [2048, 1024], P('sp', 'tp'), may hold values from -0.125 to 0.125
- floor_rate: float32 [1024], P('tp'), as said below
- extra_logdecay: float32 [4096, 8], P('sp', 'tp'), as said below
- state_gain: float32 [1024], P('tp'), may hold values from 0.1 to 1.9
- pool_mix: bfloat16 [8, 128, 128], P('tp'), may hold values from -0.5 to 0.5
- pool_gain: float32 [1024], P('tp'), may hold values from 0.1 to 1.9
- out_rec: bfloat16 [1024, 2048], P('tp', 'sp'), may hold values from -0.125 to 0.125
- out_pool: bfloat16 [1024, 2048], P('tp', 'sp'), may hold values from -0.125 to 0.125
- post_gain: float32 [2048], replicated, may hold values from 0.1 to 1.9
Outputs:
- mixed_out: bfloat16 [4096, 2048], P(('sp', 'tp'))
The draws below stay inside these ranges and needn't reach their ends.
Inputs may be any that keep to these rules, and one draw needn't show every extreme that they name: `floor_rate`: every entry is positive. `extra_logdecay`: every entry is at most zero.
All inputs are finite; a program needn't handle non-finite values.
Results may differ from the reference program's by a relative error of at most 0.015.
Values may be sent and summed in bfloat16 or wider, within the bound.
A program may use at most 64 MiB of HBM per device.

```python
import math
import jax
import jax.numpy as jnp
from jax import lax

D = 2048
HEADS = 8
DK = 128
BLOCK = 64
TOK_DEV = 256
W = 1024
TOKENS = 4096
N_TP = 2


def draw_tokens_in(key, part):
    first, second, third = jax.random.split(jax.random.fold_in(key, 3), 3)
    row_scale = jnp.exp(jax.random.uniform(first, (TOKENS, 1), jnp.float32) * math.log(10.0))
    col_scale = jnp.exp(jax.random.uniform(second, (1, D), jnp.float32) * math.log(10.0))
    starting_shift_amount = jax.random.normal(third, (TOKENS, D), jnp.float32)
    starting_shift_amount = jnp.clip(starting_shift_amount, -4.0, 4.0)
    return (starting_shift_amount * row_scale * col_scale).astype(jnp.bfloat16)


def draw_floor_rate(key, part):
    first, second = jax.random.split(jax.random.fold_in(key, 11), 2)
    ranks = jax.random.permutation(first, HEADS)
    uniform = jax.random.uniform(second, (HEADS, DK), jnp.float32)
    kind = jnp.where(ranks < HEADS // 4, 0, jnp.where(ranks < HEADS // 2, 1, 2))
    fast = jnp.exp(math.log(0.02) + uniform * math.log(4.0))
    medium_low = min(1.0 / TOK_DEV, 0.01)
    medium = jnp.exp(math.log(medium_low) + uniform * math.log(8.0))
    slow = jnp.exp(jnp.log(0.3 / TOKENS) + uniform * math.log(4.0 / 0.3))
    rate = jnp.where(kind[:, None] == 0, fast, jnp.where(kind[:, None] == 1, medium, slow))
    rate = jnp.minimum(rate, 0.08)
    return rate.reshape(HEADS * DK).astype(jnp.float32)


def draw_extra_logdecay(key, part):
    first, second, third = jax.random.split(jax.random.fold_in(key, 17), 3)
    devices = TOKENS // TOK_DEV
    factor = jnp.exp(math.log(0.3) + jax.random.uniform(first, (devices,), jnp.float32) * math.log(10.0))
    starting_shift_amount = -jnp.repeat(factor, TOK_DEV)[:, None] / TOKENS * jnp.ones((1, HEADS), jnp.float32)
    averaging_locations = jax.random.randint(second, (4, HEADS), 0, TOKENS)
    sigmoid_weighting = jnp.log(jax.random.uniform(third, (4, HEADS), jnp.float32, 0.5, 0.8))
    sequence_step_number = jnp.arange(TOKENS)[:, None, None]
    packet_clusters = jnp.sum(jnp.where(sequence_step_number == averaging_locations[None, :, :], sigmoid_weighting[None, :, :], 0.0), axis=1)
    return (starting_shift_amount + packet_clusters).astype(jnp.float32)


def shard_levels(rng, dims, pieces, least, largest):
    gain = 1.0
    for axis_at, blocks in pieces:
        heights = jax.random.uniform(jax.random.fold_in(jax.random.fold_in(rng, 6), axis_at), (blocks,), jnp.float32, least / len(pieces), largest / len(pieces))
        gain = gain * jnp.repeat(jnp.exp(heights), dims[axis_at] // blocks).reshape((-1,) + (1,) * (len(dims) - 1 - axis_at))
    return gain


def normal_values(rng, dims, width, bound, cuts=(), held_as=jnp.bfloat16):
    drawn = jax.random.normal(rng, dims, jnp.float32) * width
    if len(cuts) > 0:
        drawn = shard_levels(rng, dims, cuts, -0.22, 0.18) * drawn
    return jnp.clip(drawn, min=-bound, max=bound).astype(held_as)


def setup_inputs(seed: int = 0) -> dict:
    arg_keys = jax.random.split(jax.random.key(seed), 17)
    return {
        "tokens_in": draw_tokens_in(jax.random.fold_in(arg_keys[16], 71), 0),
        "norm_gain": jnp.clip(1.0 + 0.18 * jax.random.normal(arg_keys[1], (D,), jnp.float32), 0.1, 1.9),
        "w_query": normal_values(arg_keys[2], (D, W), D ** -0.5, 0.125, ((0, 16), (1, 2))),
        "w_forget": normal_values(arg_keys[3], (D, W), D ** -0.5, 0.125, ((0, 16), (1, 2))),
        "w_input": normal_values(arg_keys[4], (D, W), D ** -0.5, 0.125, ((0, 16), (1, 2))),
        "w_rgate": normal_values(arg_keys[5], (D, W), D ** -0.5, 0.125, ((0, 16), (1, 2))),
        "w_pool_in": normal_values(arg_keys[6], (D, W), D ** -0.5, 0.125, ((0, 16), (1, 2))),
        "w_pgate": normal_values(arg_keys[7], (D, W), D ** -0.5, 0.125, ((0, 16), (1, 2))),
        "floor_rate": draw_floor_rate(jax.random.fold_in(arg_keys[16], 71), 0),
        "extra_logdecay": draw_extra_logdecay(jax.random.fold_in(arg_keys[16], 71), 0),
        "state_gain": jnp.clip(1.0 + 0.18 * jax.random.normal(arg_keys[10], (W,), jnp.float32), 0.1, 1.9),
        "pool_mix": normal_values(arg_keys[11], (HEADS, DK, DK), DK ** -0.5, 0.5, ((0, 2),)),
        "pool_gain": jnp.clip(1.0 + 0.18 * jax.random.normal(arg_keys[12], (W,), jnp.float32), 0.1, 1.9),
        "out_rec": normal_values(arg_keys[13], (W, D), (2 * W) ** -0.5, 0.125, ((0, 2), (1, 16))),
        "out_pool": normal_values(arg_keys[14], (W, D), (2 * W) ** -0.5, 0.125, ((0, 2), (1, 16))),
        "post_gain": jnp.clip(1.0 + 0.18 * jax.random.normal(arg_keys[15], (D,), jnp.float32), 0.1, 1.9),
    }


eps = 1e-06
coarsest_scale_depth = lax.Precision.HIGHEST

def recurrence(query, key_gate, inputs, log_forget):
    blocks = TOKENS // BLOCK

    def to_blocks(array):
        return array.reshape(blocks, BLOCK, HEADS, DK).transpose(0, 2, 1, 3)
    causal = jnp.arange(BLOCK)[:, None] >= jnp.arange(BLOCK)[None, :]

    def advance(carried_memory_matrix, member):
        probe_segment, key_piece, input_piece, gc = member
        prefix_sum_vector = jnp.cumsum(gc, axis=1)
        last_index = prefix_sum_vector[:, -1]
        cross_segment_contribution = jnp.einsum('abz,azy->aby', probe_segment * jnp.exp(prefix_sum_vector), carried_memory_matrix, precision=coarsest_scale_depth)
        diff = prefix_sum_vector[:, :, None, :] - prefix_sum_vector[:, None, :, :]
        weight = jnp.where(causal[None, :, :, None], jnp.exp(jnp.minimum(diff, 0.0)), 0.0)
        scores = jnp.einsum('htk,hsk,htsk->hts', probe_segment, key_piece, weight, precision=coarsest_scale_depth)
        final_result = cross_segment_contribution + jnp.einsum('hts,hsv->htv', scores, input_piece, precision=coarsest_scale_depth)
        carried_memory_matrix = jnp.exp(last_index)[..., None] * carried_memory_matrix + jnp.einsum('njp,njq->npq', key_piece * jnp.exp(last_index[:, None, :] - prefix_sum_vector), input_piece, precision=coarsest_scale_depth)
        return (carried_memory_matrix, final_result)
    start = jnp.zeros((HEADS, DK, DK), jnp.float32)
    qs = query.astype(jnp.float32) * DK ** (-0.5)
    _, final_result = lax.scan(advance, start, (to_blocks(qs), to_blocks(key_gate), to_blocks(inputs.astype(jnp.float32)), to_blocks(log_forget)))
    return final_result.transpose(0, 2, 1, 3).reshape(TOKENS, HEADS * DK)

def reference(tokens_in, norm_gain, w_query, w_forget, w_input, w_rgate, w_pool_in, w_pgate, floor_rate, extra_logdecay, state_gain, pool_mix, pool_gain, out_rec, out_pool, post_gain):
    wide = tokens_in.astype(jnp.float32)
    inv_rms = lax.rsqrt(lax.optimization_barrier(jnp.mean(wide * wide, axis=1, keepdims=True)) + eps)
    scaled = (wide * norm_gain).astype(jnp.bfloat16)

    def project(weight):
        return (jnp.dot(scaled, weight, preferred_element_type=jnp.float32) * inv_rms).astype(jnp.bfloat16)
    query = project(w_query)
    forget = project(w_forget)
    inputs = project(w_input)
    rgate = project(w_rgate)
    pool_in = project(w_pool_in)
    pgate = project(w_pgate)
    forget32 = forget.astype(jnp.float32)
    key_gate = -jnp.expm1(-floor_rate)[None, :] * jax.nn.sigmoid(-forget32)
    log_forget = jnp.log1p(-key_gate) + jnp.repeat(extra_logdecay, DK, axis=1)
    recurrent_output = recurrence(query, key_gate, inputs, log_forget)
    grouped = recurrent_output.reshape(TOKENS, HEADS, DK)
    normed = grouped * lax.rsqrt(lax.optimization_barrier(jnp.mean(grouped * grouped, axis=2, keepdims=True)) + eps)
    y_rec = (normed.reshape(TOKENS, HEADS * DK) * state_gain * jax.nn.silu(rgate.astype(jnp.float32))).astype(jnp.bfloat16)
    group = (jnp.arange(HEADS * DK) // DK).astype(jnp.int32)
    window = jnp.power(2, 1 + group % 4).astype(jnp.int32)
    pool32 = pool_in.astype(jnp.float32)
    extended = jnp.concatenate([jnp.zeros((16, HEADS * DK), jnp.float32), pool32], axis=0)
    total = jnp.zeros((TOKENS, HEADS * DK), jnp.float32)
    for offset in range(16):
        rows_back = extended[16 - offset:16 - offset + TOKENS]
        total = total + jnp.where((offset < window)[None, :], rows_back, 0.0)
    sequence_step_number = jnp.arange(TOKENS).astype(jnp.int32)
    count = jnp.minimum(sequence_step_number[:, None] + 1, window[None, :]).astype(jnp.float32)
    mixed = (total / count - pool32).astype(jnp.bfloat16)
    mapped = jnp.einsum('tgc,gcd->tgd', mixed.reshape(TOKENS, HEADS, DK).astype(jnp.float32), pool_mix.astype(jnp.float32)).reshape(TOKENS, HEADS * DK)
    y_pool = (mapped * pool_gain * jax.nn.silu(pgate.astype(jnp.float32))).astype(jnp.bfloat16)
    share = HEADS * DK // N_TP
    summed = jnp.zeros((TOKENS, D), jnp.float32)
    for member in range(N_TP):
        lower = member * share
        left = jnp.concatenate([y_rec[:, lower:lower + share], y_pool[:, lower:lower + share]], axis=1)
        right = jnp.concatenate([out_rec[lower:lower + share], out_pool[lower:lower + share]], axis=0)
        partial_sum = jnp.dot(left, right, preferred_element_type=jnp.float32).astype(jnp.bfloat16)
        summed = summed + partial_sum.astype(jnp.float32)
    final = summed * lax.rsqrt(lax.optimization_barrier(jnp.mean(summed * summed, axis=1, keepdims=True)) + eps) * post_gain
    return final.astype(jnp.bfloat16)
```

```python
import jax
import jax.numpy as jnp
from jax import lax
from jax.experimental import pallas as pl
from jax.experimental.pallas import tpu as pltpu
from jax.sharding import PartitionSpec as P

DK = 128
BLOCK = 64


eps = 1e-06
coarsest_scale_depth = lax.Precision.HIGHEST


def prefix(part, axis, combine, identity):
    place = lax.axis_index(axis)
    gathered = jax.tree.map(lambda a: lax.all_gather(a, axis), part)
    state = jax.tree.map(lambda a, e: jnp.zeros_like(a) + jnp.asarray(e, a.dtype), part, identity)

    def one(turn, state):
        return combine(
            state, jax.tree.map(lambda a: lax.dynamic_index_in_dim(a, turn, 0, False), gathered)
        )

    return lax.fori_loop(0, place, one, state)


def shifted(value, axis, steps):
    count = lax.axis_size(axis)
    initial, last = (max(0, -steps), min(count, count - steps))
    return lax.ppermute(value, axis, [(source, source + steps) for source in range(initial, last)])


PIECES = 2


def ring_place(chip, chips):
    odd = chip % 2
    return (1 - odd) * (chip // 2) + odd * (chips - 1 - chip // 2)


def ring_chip(place, chips):
    back = place // (chips // 2)
    return (1 - back) * (2 * place) + back * (2 * (chips - 1 - place) + 1)


def project_kernel(
    n,
    n_tp,
    tok_ref,
    gain_ref,
    w_ref,
    proj_ref,
    wide,
    scaled,
    weights,
    acc,
    tok_send,
    tok_recv,
    own_sem,
    ring_send,
    ring_recv,
    core_send,
    core_recv,
):
    chips = n // 2
    steps = chips // 2
    me = lax.axis_index("sp")
    tp = lax.axis_index("tp")
    core = me % 2
    place = ring_place(me // 2, chips)

    def chip_at(offset):
        return ring_chip((place + offset + chips) % chips, chips)

    following = 2 * chip_at(1) + core
    preceding = 2 * chip_at(-1) + core
    partner = 2 * (me // 2) + 1 - core
    rows = w_ref.shape[0]
    piece = rows // PIECES
    features = tok_ref.shape[1]

    barrier = pltpu.get_barrier_semaphore()
    for peer in (following, preceding, partner):
        pl.semaphore_signal(barrier, inc=1, device_id={"sp": peer})
    for turn in range(1, n_tp):
        pl.semaphore_signal(barrier, inc=1, device_id={"tp": (tp + turn) % n_tp})
    pl.semaphore_wait(barrier, 3 + n_tp - 1)

    def rows_of(chip, which, q):
        start = (2 * chip + which) * rows + q * piece
        return pl.ds(pl.multiple_of(start, 16), piece)

    sends = []

    def to_core(offset, q, source):
        slot = offset + steps - 1
        copy = pltpu.make_async_remote_copy(
            src_ref=source,
            dst_ref=weights.at[rows_of(chip_at(offset), core, q)],
            send_sem=core_send.at[slot, q],
            recv_sem=core_recv.at[slot, q],
            device_id={"sp": partner},
        )
        copy.start()
        sends.append(copy)

    def from_core(offset, q):
        slot = offset + steps - 1
        dst = weights.at[rows_of(chip_at(offset), 1 - core, q)]
        pltpu.make_async_remote_copy(
            src_ref=dst,
            dst_ref=dst,
            send_sem=core_send.at[slot, q],
            recv_sem=core_recv.at[slot, q],
            device_id={"sp": partner},
        ).wait_recv()

    def pieces_of(direction, step):
        if step < steps - 1:
            return range(PIECES)
        half = PIECES // 2
        return range(half) if direction == 0 else range(half, PIECES)

    def ring_copy(direction, step, q, source):
        offset = -step if direction == 0 else step
        dst = weights.at[rows_of(chip_at(offset), core, q)]
        return pltpu.make_async_remote_copy(
            src_ref=dst if source is None else source,
            dst_ref=dst,
            send_sem=ring_send.at[direction, step, q],
            recv_sem=ring_recv.at[direction, step, q],
            device_id={"sp": following if direction == 0 else preceding},
        )

    def ring_arrival(direction, step, q):
        offset = -(step + 1) if direction == 0 else step + 1
        dst = weights.at[rows_of(chip_at(offset), core, q)]
        pltpu.make_async_remote_copy(
            src_ref=dst,
            dst_ref=dst,
            send_sem=ring_send.at[direction, step, q],
            recv_sem=ring_recv.at[direction, step, q],
            device_id={"sp": following if direction == 0 else preceding},
        ).wait_recv()

    for q in range(PIECES):
        mine = w_ref.at[pl.ds(q * piece, piece)]
        for direction in range(2):
            if q in pieces_of(direction, 0):
                copy = ring_copy(direction, 0, q, mine)
                copy.start()
                sends.append(copy)
        to_core(0, q, mine)
    tokens_at = pl.ds(pl.multiple_of(tp * features, 128), features)
    for turn in range(1, n_tp):
        copy = pltpu.make_async_remote_copy(
            src_ref=tok_ref,
            dst_ref=wide.at[:, tokens_at],
            send_sem=tok_send.at[turn - 1],
            recv_sem=tok_recv.at[turn - 1],
            device_id={"tp": (tp + turn) % n_tp},
        )
        copy.start()
        sends.append(copy)
    own = pltpu.make_async_copy(
        w_ref, weights.at[pl.ds(pl.multiple_of(me * rows, 16), rows)], own_sem
    )
    own.start()
    acc[...] = jnp.zeros_like(acc)
    wide[:, tokens_at] = tok_ref[...]
    for turn in range(1, n_tp):
        theirs = pl.ds(
            pl.multiple_of((tp - turn + n_tp) % n_tp * features, 128), features
        )
        pltpu.make_async_remote_copy(
            src_ref=tok_ref,
            dst_ref=wide.at[:, theirs],
            send_sem=tok_send.at[turn - 1],
            recv_sem=tok_recv.at[turn - 1],
            device_id={"tp": (tp + turn) % n_tp},
        ).wait_recv()
    scaled[...] = (wide[...].astype(jnp.float32) * gain_ref[...]).astype(jnp.bfloat16)

    cols = weights.shape[1]
    tile = cols // 6

    by_chip = (2 * rows) % 128 == 0

    def multiply(offset):
        if not by_chip:
            return
        multiply_rows(pl.ds(pl.multiple_of(chip_at(offset) * 2 * rows, 2 * rows), 2 * rows))

    def multiply_rows(depth):
        def one(i, _):
            at = pl.ds(pl.multiple_of(i * tile, 128), tile)
            acc[:, at] += jnp.dot(
                scaled[:, depth], weights[depth, at], preferred_element_type=jnp.float32
            )
            return 0

        lax.fori_loop(0, 6, one, 0)

    own.wait()
    for step in range(steps):
        for q in range(PIECES):
            for direction in range(2):
                if q not in pieces_of(direction, step):
                    continue
                offset = -(step + 1) if direction == 0 else step + 1
                ring_arrival(direction, step, q)
                if step + 1 < steps and q in pieces_of(direction, step + 1):
                    copy = ring_copy(direction, step + 1, q, None)
                    copy.start()
                    sends.append(copy)
                last = offset if abs(offset) < steps else steps
                dst = weights.at[rows_of(chip_at(last), core, q)]
                to_core(last, q, dst)
        for offset in [0] if step == 0 else [-step, step]:
            for q in range(PIECES):
                from_core(offset, q)
            multiply(offset)
    for q in range(PIECES):
        from_core(steps, q)
    multiply(steps)
    if not by_chip:
        multiply_rows(slice(None))
    values = wide[...].astype(jnp.float32)
    squares = jnp.sum(values * values, axis=1, keepdims=True)
    inv_rms = lax.rsqrt(squares / wide.shape[1] + eps)
    proj_ref[...] = (acc[...] * inv_rms).astype(jnp.bfloat16)
    for copy in sends:
        copy.wait_send()


def project(tokens, gain, shard):
    import functools

    n = lax.axis_size("sp")
    n_tp = lax.axis_size("tp")
    positions, features = tokens.shape
    rows, cols = shard.shape
    width = n * rows
    steps = n // 4
    dma = pltpu.SemaphoreType.DMA
    return pl.pallas_call(
        functools.partial(project_kernel, n, n_tp),
        out_shape=jax.ShapeDtypeStruct((positions, cols), jnp.bfloat16),
        in_specs=[pl.BlockSpec(memory_space=pltpu.VMEM)] * 3,
        out_specs=pl.BlockSpec(memory_space=pltpu.VMEM),
        scratch_shapes=[
            pltpu.VMEM((positions, width), jnp.bfloat16),
            pltpu.VMEM((positions, width), jnp.bfloat16),
            pltpu.VMEM((width, cols), jnp.bfloat16),
            pltpu.VMEM((positions, cols), jnp.float32),
            dma((n_tp,)),
            dma((n_tp,)),
            dma,
            dma((2, steps, PIECES)),
            dma((2, steps, PIECES)),
            dma((2 * steps, PIECES)),
            dma((2 * steps, PIECES)),
        ],
        compiler_params=pltpu.CompilerParams(
            collective_id=0, has_side_effects=True, vmem_limit_bytes=56 * 1024 * 1024
        ),
        cost_estimate=pl.CostEstimate(
            flops=2 * positions * width * cols, bytes_accessed=4 * rows * cols, transcendentals=0
        ),
    )(tokens, gain[None, :], shard)


def chain_merge(earlier, later):
    return (earlier[0] * later[0], later[0][..., None] * earlier[1] + later[1])


def local_blocks(qs, keys, values, logs):
    causal = jnp.arange(BLOCK)[:, None] >= jnp.arange(BLOCK)[None, :]
    heads_dev = qs.shape[1]

    def advance(carry, member):
        carried_memory_matrix, start = carry
        probe_segment, key_piece, input_piece, gc = member
        prefix_sum_vector = jnp.cumsum(gc, axis=1)
        last_index = prefix_sum_vector[:, -1]
        cross_segment_contribution = jnp.einsum(
            "abz,azy->aby",
            probe_segment * jnp.exp(prefix_sum_vector),
            carried_memory_matrix,
            precision=coarsest_scale_depth,
        )
        diff = prefix_sum_vector[:, :, None, :] - prefix_sum_vector[:, None, :, :]
        weight = jnp.where(causal[None, :, :, None], jnp.exp(jnp.minimum(diff, 0.0)), 0.0)
        scores = jnp.einsum(
            "htk,hsk,htsk->hts", probe_segment, key_piece, weight, precision=coarsest_scale_depth
        )
        final_result = cross_segment_contribution + jnp.einsum(
            "hts,hsv->htv", scores, input_piece, precision=coarsest_scale_depth
        )
        carried_memory_matrix = jnp.exp(last_index)[..., None] * carried_memory_matrix + jnp.einsum(
            "njp,njq->npq",
            key_piece * jnp.exp(last_index[:, None, :] - prefix_sum_vector),
            input_piece,
            precision=coarsest_scale_depth,
        )
        pool_reach = probe_segment * jnp.exp(start[:, None, :] + prefix_sum_vector)
        return ((carried_memory_matrix, start + last_index), (final_result, pool_reach))

    begin = (jnp.zeros((heads_dev, DK, DK), jnp.float32), jnp.zeros((heads_dev, DK), jnp.float32))
    (carried_memory_matrix, total), (final_result, pool_reach) = lax.scan(
        advance, begin, (qs, keys, values, logs)
    )
    return (carried_memory_matrix, total, final_result, pool_reach)


def per_device(
    tokens_in,
    norm_gain,
    w_query,
    w_forget,
    w_input,
    w_rgate,
    w_pool_in,
    w_pgate,
    floor_rate,
    extra_logdecay,
    state_gain,
    pool_mix,
    pool_gain,
    out_rec,
    out_pool,
    post_gain,
):
    shard = jnp.concatenate(
        [w_query, w_forget, w_input, w_rgate, w_pool_in, w_pgate], axis=1
    )
    head_cols = w_query.shape[1]
    positions = tokens_in.shape[0]
    proj = project(tokens_in, norm_gain, shard)
    query = proj[:, 0:head_cols]
    forget = proj[:, head_cols : 2 * head_cols]
    inputs = proj[:, 2 * head_cols : 3 * head_cols]
    rgate = proj[:, 3 * head_cols : 4 * head_cols]
    pool_in = proj[:, 4 * head_cols : 5 * head_cols]
    pgate = proj[:, 5 * head_cols : 6 * head_cols]
    heads_dev = head_cols // DK
    blocks = positions // BLOCK

    def to_blocks(array):
        return array.reshape(blocks, BLOCK, heads_dev, DK).transpose(0, 2, 1, 3)

    forget32 = forget.astype(jnp.float32)
    key_gate = -jnp.expm1(-floor_rate)[None, :] * jax.nn.sigmoid(-forget32)
    log_forget = jnp.log1p(-key_gate) + jnp.repeat(extra_logdecay, DK, axis=1)
    qs = query.astype(jnp.float32) * DK ** (-0.5)
    carried_memory_matrix, total, final_result, pool_reach = local_blocks(
        to_blocks(qs),
        to_blocks(key_gate),
        to_blocks(inputs.astype(jnp.float32)),
        to_blocks(log_forget),
    )
    decays = jnp.exp(total)
    tail_rows = pool_in[positions - 16 :]
    carried = prefix(
        (decays, carried_memory_matrix),
        "sp",
        chain_merge,
        (jnp.ones_like(decays), jnp.zeros_like(carried_memory_matrix)),
    )
    incoming_state = carried[1]
    previous = shifted(tail_rows, "sp", 1).astype(jnp.float32)
    recurrent_output = final_result + jnp.einsum(
        "izaf,zfu->izau", pool_reach, incoming_state, precision=coarsest_scale_depth
    )
    grouped = recurrent_output.transpose(0, 2, 1, 3).reshape(positions, heads_dev, DK)
    normed = grouped * lax.rsqrt(jnp.mean(grouped * grouped, axis=2, keepdims=True) + eps)
    y_rec = (
        normed.reshape(positions, head_cols)
        * state_gain[None, :]
        * jax.nn.silu(rgate.astype(jnp.float32))
    ).astype(jnp.bfloat16)
    group = lax.axis_index("tp") * heads_dev + jnp.arange(head_cols) // DK
    window = jnp.power(2, 1 + group % 4).astype(jnp.int32)
    pool32 = pool_in.astype(jnp.float32)
    extended = jnp.concatenate([previous, pool32], axis=0)
    summed_rows = jnp.zeros((positions, head_cols), jnp.float32)
    for offset in range(16):
        rows_back = extended[16 - offset : 16 - offset + positions]
        summed_rows = summed_rows + jnp.where((offset < window)[None, :], rows_back, 0.0)
    place = lax.axis_index("sp") * positions + jnp.arange(positions)
    count = jnp.minimum(place[:, None] + 1, window[None, :]).astype(jnp.float32)
    mixed = (summed_rows / count - pool32).astype(jnp.bfloat16)
    mapped = jnp.einsum(
        "tgc,gcd->tgd",
        mixed.reshape(positions, heads_dev, DK),
        pool_mix,
        preferred_element_type=jnp.float32,
    ).reshape(positions, head_cols)
    y_pool = (mapped * pool_gain[None, :] * jax.nn.silu(pgate.astype(jnp.float32))).astype(
        jnp.bfloat16
    )
    out_parts = (
        lax.all_gather(out_rec, "sp", axis=1, tiled=True),
        lax.all_gather(out_pool, "sp", axis=1, tiled=True),
    )
    both = jnp.concatenate([y_rec, y_pool], axis=1)
    weight_cat = jnp.concatenate(out_parts, axis=0)
    summed = lax.psum_scatter(
        jnp.dot(both, weight_cat, preferred_element_type=jnp.float32).astype(jnp.bfloat16),
        "tp",
        scatter_dimension=0,
        tiled=True,
    ).astype(jnp.float32)
    final = (
        summed
        * lax.rsqrt(jnp.mean(summed * summed, axis=1, keepdims=True) + eps)
        * post_gain[None, :]
    )
    return final.astype(jnp.bfloat16)


def solution(mesh):
    placed = (
        P("sp", "tp"),
        P(),
        P("sp", "tp"),
        P("sp", "tp"),
        P("sp", "tp"),
        P("sp", "tp"),
        P("sp", "tp"),
        P("sp", "tp"),
        P("tp"),
        P("sp", "tp"),
        P("tp"),
        P("tp", None, None),
        P("tp"),
        P("tp", "sp"),
        P("tp", "sp"),
        P(),
    )
    return jax.shard_map(
        per_device, mesh=mesh, in_specs=placed, out_specs=P(("sp", "tp"), None), check_vma=False
    )
```

```python
import functools

import jax
import jax.numpy as jnp
from jax import lax
from jax.experimental import pallas as pl
from jax.experimental.pallas import tpu as pltpu
from jax.sharding import PartitionSpec as P

DK = 128


eps = 1e-06
coarsest_scale_depth = lax.Precision.HIGHEST


PIECES = 2


def ring_place(chip, chips):
    odd = chip % 2
    return (1 - odd) * (chip // 2) + odd * (chips - 1 - chip // 2)


def ring_chip(place, chips):
    back = place // (chips // 2)
    return (1 - back) * (2 * place) + back * (2 * (chips - 1 - place) + 1)


def project_kernel(
    n,
    n_tp,
    tok_ref,
    gain_ref,
    w_ref,
    proj_ref,
    wide,
    scaled,
    weights,
    acc,
    tok_send,
    tok_recv,
    own_sem,
    ring_send,
    ring_recv,
    core_send,
    core_recv,
):
    chips = n // 2
    steps = chips // 2
    me = lax.axis_index("sp")
    tp = lax.axis_index("tp")
    core = me % 2
    place = ring_place(me // 2, chips)

    def chip_at(offset):
        return ring_chip((place + offset + chips) % chips, chips)

    following = 2 * chip_at(1) + core
    preceding = 2 * chip_at(-1) + core
    partner = 2 * (me // 2) + 1 - core
    rows = w_ref.shape[0]
    piece = rows // PIECES
    features = tok_ref.shape[1]

    barrier = pltpu.get_barrier_semaphore()
    for peer in (following, preceding, partner):
        pl.semaphore_signal(barrier, inc=1, device_id={"sp": peer})
    for turn in range(1, n_tp):
        pl.semaphore_signal(barrier, inc=1, device_id={"tp": (tp + turn) % n_tp})
    pl.semaphore_wait(barrier, 3 + n_tp - 1)

    def rows_of(chip, which, q):
        start = (2 * chip + which) * rows + q * piece
        return pl.ds(pl.multiple_of(start, 16), piece)

    sends = []

    def to_core(offset, q, source):
        slot = offset + steps - 1
        copy = pltpu.make_async_remote_copy(
            src_ref=source,
            dst_ref=weights.at[rows_of(chip_at(offset), core, q)],
            send_sem=core_send.at[slot, q],
            recv_sem=core_recv.at[slot, q],
            device_id={"sp": partner},
        )
        copy.start()
        sends.append(copy)

    def from_core(offset, q):
        slot = offset + steps - 1
        dst = weights.at[rows_of(chip_at(offset), 1 - core, q)]
        pltpu.make_async_remote_copy(
            src_ref=dst,
            dst_ref=dst,
            send_sem=core_send.at[slot, q],
            recv_sem=core_recv.at[slot, q],
            device_id={"sp": partner},
        ).wait_recv()

    def pieces_of(direction, step):
        if step < steps - 1:
            return range(PIECES)
        half = PIECES // 2
        return range(half) if direction == 0 else range(half, PIECES)

    def ring_copy(direction, step, q, source):
        offset = -step if direction == 0 else step
        dst = weights.at[rows_of(chip_at(offset), core, q)]
        return pltpu.make_async_remote_copy(
            src_ref=dst if source is None else source,
            dst_ref=dst,
            send_sem=ring_send.at[direction, step, q],
            recv_sem=ring_recv.at[direction, step, q],
            device_id={"sp": following if direction == 0 else preceding},
        )

    def ring_arrival(direction, step, q):
        offset = -(step + 1) if direction == 0 else step + 1
        dst = weights.at[rows_of(chip_at(offset), core, q)]
        pltpu.make_async_remote_copy(
            src_ref=dst,
            dst_ref=dst,
            send_sem=ring_send.at[direction, step, q],
            recv_sem=ring_recv.at[direction, step, q],
            device_id={"sp": following if direction == 0 else preceding},
        ).wait_recv()

    for q in range(PIECES):
        mine = w_ref.at[pl.ds(q * piece, piece)]
        for direction in range(2):
            if q in pieces_of(direction, 0):
                copy = ring_copy(direction, 0, q, mine)
                copy.start()
                sends.append(copy)
        to_core(0, q, mine)
    tokens_at = pl.ds(pl.multiple_of(tp * features, 128), features)
    for turn in range(1, n_tp):
        copy = pltpu.make_async_remote_copy(
            src_ref=tok_ref,
            dst_ref=wide.at[:, tokens_at],
            send_sem=tok_send.at[turn - 1],
            recv_sem=tok_recv.at[turn - 1],
            device_id={"tp": (tp + turn) % n_tp},
        )
        copy.start()
        sends.append(copy)
    own = pltpu.make_async_copy(
        w_ref, weights.at[pl.ds(pl.multiple_of(me * rows, 16), rows)], own_sem
    )
    own.start()
    acc[...] = jnp.zeros_like(acc)
    wide[:, tokens_at] = tok_ref[...]
    for turn in range(1, n_tp):
        theirs = pl.ds(
            pl.multiple_of((tp - turn + n_tp) % n_tp * features, 128), features
        )
        pltpu.make_async_remote_copy(
            src_ref=tok_ref,
            dst_ref=wide.at[:, theirs],
            send_sem=tok_send.at[turn - 1],
            recv_sem=tok_recv.at[turn - 1],
            device_id={"tp": (tp + turn) % n_tp},
        ).wait_recv()
    scaled[...] = (wide[...].astype(jnp.float32) * gain_ref[...]).astype(jnp.bfloat16)

    cols = weights.shape[1]
    tile = cols // 6

    by_chip = (2 * rows) % 128 == 0

    def multiply(offset):
        if not by_chip:
            return
        multiply_rows(pl.ds(pl.multiple_of(chip_at(offset) * 2 * rows, 2 * rows), 2 * rows))

    def multiply_rows(depth):
        def one(i, _):
            at = pl.ds(pl.multiple_of(i * tile, 128), tile)
            acc[:, at] += jnp.dot(
                scaled[:, depth], weights[depth, at], preferred_element_type=jnp.float32
            )
            return 0

        lax.fori_loop(0, 6, one, 0)

    own.wait()
    for step in range(steps):
        for q in range(PIECES):
            for direction in range(2):
                if q not in pieces_of(direction, step):
                    continue
                offset = -(step + 1) if direction == 0 else step + 1
                ring_arrival(direction, step, q)
                if step + 1 < steps and q in pieces_of(direction, step + 1):
                    copy = ring_copy(direction, step + 1, q, None)
                    copy.start()
                    sends.append(copy)
                last = offset if abs(offset) < steps else steps
                dst = weights.at[rows_of(chip_at(last), core, q)]
                to_core(last, q, dst)
        for offset in [0] if step == 0 else [-step, step]:
            for q in range(PIECES):
                from_core(offset, q)
            multiply(offset)
    for q in range(PIECES):
        from_core(steps, q)
    multiply(steps)
    if not by_chip:
        multiply_rows(slice(None))
    values = wide[...].astype(jnp.float32)
    squares = jnp.sum(values * values, axis=1, keepdims=True)
    inv_rms = lax.rsqrt(squares / wide.shape[1] + eps)
    proj_ref[...] = (acc[...] * inv_rms).astype(jnp.bfloat16)
    for copy in sends:
        copy.wait_send()


def project(tokens, gain, shard):
    n = lax.axis_size("sp")
    n_tp = lax.axis_size("tp")
    positions, features = tokens.shape
    rows, cols = shard.shape
    width = n * rows
    steps = n // 4
    dma = pltpu.SemaphoreType.DMA
    return pl.pallas_call(
        functools.partial(project_kernel, n, n_tp),
        out_shape=jax.ShapeDtypeStruct((positions, cols), jnp.bfloat16),
        in_specs=[pl.BlockSpec(memory_space=pltpu.VMEM)] * 3,
        out_specs=pl.BlockSpec(memory_space=pltpu.VMEM),
        scratch_shapes=[
            pltpu.VMEM((positions, width), jnp.bfloat16),
            pltpu.VMEM((positions, width), jnp.bfloat16),
            pltpu.VMEM((width, cols), jnp.bfloat16),
            pltpu.VMEM((positions, cols), jnp.float32),
            dma((n_tp,)),
            dma((n_tp,)),
            dma,
            dma((2, steps, PIECES)),
            dma((2, steps, PIECES)),
            dma((2 * steps, PIECES)),
            dma((2 * steps, PIECES)),
        ],
        compiler_params=pltpu.CompilerParams(
            collective_id=0, has_side_effects=True, vmem_limit_bytes=56 * 1024 * 1024
        ),
        cost_estimate=pl.CostEstimate(
            flops=2 * positions * width * cols, bytes_accessed=4 * rows * cols, transcendentals=0
        ),
    )(tokens, gain[None, :], shard)


def mix_kernel(
    n,
    n_tp,
    proj_ref,
    keep_ref,
    extra_ref,
    sgain_ref,
    mix_ref,
    pgain_ref,
    w_ref,
    post_ref,
    out_ref,
    weights,
    local,
    reach,
    both,
    state,
    before,
    gone_state,
    gone_decay,
    come_state,
    come_decay,
    tail,
    tail_in,
    mine,
    gone_out,
    come_out,
    ring_send,
    ring_recv,
    core_send,
    core_recv,
    scan_send,
    scan_recv,
    tail_sem,
    own_sem,
    out_send,
    out_recv,
):
    f32, bf16 = jnp.float32, jnp.bfloat16
    chips = n // 2
    steps = chips // 2
    rounds = (n - 1).bit_length()
    me = lax.axis_index("sp")
    tp = lax.axis_index("tp")
    core = me % 2
    place = ring_place(me // 2, chips)

    def chip_at(offset):
        return ring_chip((place + offset + chips) % chips, chips)

    following = 2 * chip_at(1) + core
    preceding = 2 * chip_at(-1) + core
    partner = 2 * (me // 2) + 1 - core
    piece = w_ref.shape[0] // PIECES

    barrier = pltpu.get_barrier_semaphore()
    for peer in (following, preceding, partner):
        pl.semaphore_signal(barrier, inc=1, device_id={"sp": peer})
    for r in range(rounds):
        pl.semaphore_signal(barrier, inc=1, device_id={"sp": (me + 2**r) % n})
        pl.semaphore_signal(barrier, inc=1, device_id={"sp": (me - 2**r + n) % n})
    for turn in range(1, n_tp):
        pl.semaphore_signal(barrier, inc=1, device_id={"tp": (tp + turn) % n_tp})
    pl.semaphore_wait(barrier, 3 + 2 * rounds + n_tp - 1)

    sends = []

    def spot(chip, which, q):
        return weights.at[2 * chip + which, pl.ds(q * piece, piece)]

    def to_core(offset, q, source):
        slot = offset + steps - 1
        copy = pltpu.make_async_remote_copy(
            src_ref=source,
            dst_ref=spot(chip_at(offset), core, q),
            send_sem=core_send.at[slot, q],
            recv_sem=core_recv.at[slot, q],
            device_id={"sp": partner},
        )
        copy.start()
        sends.append(copy)

    def from_core(offset, q):
        slot = offset + steps - 1
        dst = spot(chip_at(offset), 1 - core, q)
        pltpu.make_async_remote_copy(
            src_ref=dst,
            dst_ref=dst,
            send_sem=core_send.at[slot, q],
            recv_sem=core_recv.at[slot, q],
            device_id={"sp": partner},
        ).wait_recv()

    def pieces_of(direction, step):
        if step < steps - 1:
            return range(PIECES)
        half = PIECES // 2
        return range(half) if direction == 0 else range(half, PIECES)

    def ring_copy(direction, step, q, source, offset):
        dst = spot(chip_at(offset), core, q)
        return pltpu.make_async_remote_copy(
            src_ref=dst if source is None else source,
            dst_ref=dst,
            send_sem=ring_send.at[direction, step, q],
            recv_sem=ring_recv.at[direction, step, q],
            device_id={"sp": following if direction == 0 else preceding},
        )

    def ring_step(step):
        for q in range(PIECES):
            for direction in range(2):
                if q not in pieces_of(direction, step):
                    continue
                offset = -(step + 1) if direction == 0 else step + 1
                ring_copy(direction, step, q, None, offset).wait_recv()
                if step + 1 < steps and q in pieces_of(direction, step + 1):
                    copy = ring_copy(direction, step + 1, q, None, offset)
                    copy.start()
                    sends.append(copy)
                last = offset if abs(offset) < steps else steps
                to_core(last, q, spot(chip_at(last), core, q))

    pending = list(range(steps))

    def advance_ring():
        if pending:
            ring_step(pending.pop(0))

    positions = proj_ref.shape[0]
    head_cols = proj_ref.shape[1] // 6
    heads = head_cols // DK
    reach_back = tail.shape[0]

    tail[...] = proj_ref[positions - reach_back :, 4 * head_cols : 5 * head_cols]
    for q in range(PIECES):
        own_piece = w_ref.at[pl.ds(q * piece, piece)]
        for direction in range(2):
            if q in pieces_of(direction, 0):
                copy = ring_copy(direction, 0, q, own_piece, 0)
                copy.start()
                sends.append(copy)
        to_core(0, q, own_piece)
    own = pltpu.make_async_copy(w_ref, weights.at[me], own_sem)
    own.start()
    tail_copy = pltpu.make_async_remote_copy(
        src_ref=tail,
        dst_ref=tail_in,
        send_sem=tail_sem.at[0],
        recv_sem=tail_sem.at[1],
        device_id={"sp": (me + 1) % n},
    )
    tail_copy.start()

    row = lax.broadcasted_iota(jnp.int32, (positions, positions), 0)
    col = lax.broadcasted_iota(jnp.int32, (positions, positions), 1)
    lower = jnp.where(row >= col, 1.0, 0.0).astype(f32)
    line = lax.broadcasted_iota(jnp.int32, (positions, DK), 0)
    units = positions // 8
    sub = lax.broadcasted_iota(jnp.int32, (units, 8, DK), 1)
    over_last = (((1,), (1,)), ((), ()))

    decay_now = []
    for h in range(heads):
        at = slice(h * DK, (h + 1) * DK)
        part = lambda i: proj_ref[:, i * head_cols + h * DK : i * head_cols + (h + 1) * DK]
        q = part(0).astype(f32) * DK ** (-0.5)
        kg = keep_ref[:, at] * jax.nn.sigmoid(-part(1).astype(f32))
        v = part(2)
        logs = jnp.log1p(-kg) + extra_ref[:, h : h + 1]
        c = jnp.dot(
            lower, logs, precision=coarsest_scale_depth, preferred_element_type=f32
        )
        last = c[positions - 1 :, :]
        state[h] = lax.dot_general(
            v,
            (kg * jnp.exp(last - c)).astype(bf16),
            (((0,), (0,)), ((), ())),
            preferred_element_type=f32,
        )
        gone_decay[0, h : h + 1, :] = jnp.exp(last)
        reach[:, at] = (q * jnp.exp(c)).astype(bf16)
        scores = jnp.zeros((positions, positions), f32)
        span = 8
        while span < positions:
            pair = 2 * span
            c3 = c.reshape(positions // pair, pair, DK)
            middle = jnp.broadcast_to(c3[:, span - 1 : span, :], c3.shape).reshape(c.shape)
            fade = jnp.exp(-jnp.abs(c - middle))
            later = (line // span) % 2 == 1
            probe = jnp.where(later, q * fade, 0.0).astype(bf16)
            keyed = jnp.where(later, 0.0, kg * fade).astype(bf16)
            found = lax.dot_general(probe, keyed, over_last, preferred_element_type=f32)
            scores = scores + jnp.where(row // pair == col // pair, found, 0.0)
            span = pair
        result = jnp.dot(scores.astype(bf16), v, preferred_element_type=f32)
        c3 = c.reshape(units, 8, DK)
        q3 = q.reshape(units, 8, DK)
        k3 = kg.reshape(units, 8, DK)
        v3 = v.astype(f32).reshape(units, 8, DK)
        near = result.reshape(units, 8, DK)
        for s in range(8):
            weight = jnp.exp(jnp.minimum(c3 - c3[:, s : s + 1, :], 0.0))
            score = jnp.sum(q3 * k3[:, s : s + 1, :] * weight, axis=2, keepdims=True)
            near = near + jnp.where(sub >= s, score * v3[:, s : s + 1, :], 0.0)
        local[:, at] = near.reshape(positions, DK)
        if h % 2 == 1:
            advance_ring()

    def scan_copies(r):
        target = {"sp": (me + 2**r) % n}
        return [
            pltpu.make_async_remote_copy(
                src_ref=gone.at[r],
                dst_ref=come.at[r],
                send_sem=scan_send.at[r, i],
                recv_sem=scan_recv.at[r, i],
                device_id=target,
            )
            for i, (gone, come) in enumerate(
                [(gone_state, come_state), (gone_decay, come_decay)]
            )
        ]

    before[...] = jnp.zeros_like(before)
    decay_w = [gone_decay[0, h : h + 1, :] for h in range(heads)]
    decay_e = [jnp.ones((1, DK), f32) for h in range(heads)]

    def pool(h):
        at = slice(h * DK, (h + 1) * DK)
        x = proj_ref[:, 4 * head_cols + h * DK : 4 * head_cols + (h + 1) * DK].astype(f32)
        prior = jnp.where(me > 0, tail_in[:, at].astype(f32), 0.0)
        level = (tp * heads + h) % 4
        total = jnp.concatenate([prior, x], axis=0)
        chosen = jnp.zeros((positions, DK), f32)
        for k in range(4):
            total = total + pltpu.roll(total, 2**k, 0)
            chosen = jnp.where(level == k, total[reach_back:, :], chosen)
        window = 2
        for k in range(1, 4):
            window = jnp.where(level == k, 2 ** (1 + k), window)
        count = jnp.minimum(me * positions + line + 1, window).astype(f32)
        mixed = (chosen / count - x).astype(bf16)
        mapped = jnp.dot(mixed, mix_ref[h], preferred_element_type=f32)
        gate = proj_ref[:, 5 * head_cols + h * DK : 5 * head_cols + (h + 1) * DK].astype(f32)
        both[:, head_cols + h * DK : head_cols + (h + 1) * DK] = (
            mapped * pgain_ref[:, at] * (gate * jax.nn.sigmoid(gate))
        ).astype(bf16)

    pools = list(range(heads))
    for r in range(rounds):
        gone_state[r] = state[...].astype(bf16)
        if r > 0:
            for h in range(heads):
                gone_decay[r, h : h + 1, :] = decay_w[h]
        for copy in scan_copies(r):
            copy.start()
            sends.append(copy)
        if r == 0:
            tail_copy.wait_recv()
        if pools:
            pool(pools.pop(0))
        advance_ring()
        for copy in scan_copies(r):
            copy.wait_recv()
        valid = me >= 2**r
        for h in range(heads):
            came = jnp.where(valid, come_state[r, h].astype(f32), 0.0)
            came_decay = jnp.where(valid, come_decay[r, h : h + 1, :], 1.0)
            before[h] = before[h] + decay_e[h] * came
            decay_e[h] = decay_e[h] * came_decay
            if r + 1 < rounds:
                state[h] = state[h] + decay_w[h] * came
                decay_w[h] = decay_w[h] * came_decay
    for h in pools:
        pool(h)
    while pending:
        advance_ring()

    for h in range(heads):
        at = slice(h * DK, (h + 1) * DK)
        rec = local[:, at] + lax.dot_general(
            reach[:, at], before[h].astype(bf16), over_last, preferred_element_type=f32
        )
        normed = rec * lax.rsqrt(jnp.mean(rec * rec, axis=1, keepdims=True) + eps)
        gate = proj_ref[:, 3 * head_cols + h * DK : 3 * head_cols + (h + 1) * DK].astype(f32)
        both[:, at] = (normed * sgain_ref[:, at] * (gate * jax.nn.sigmoid(gate))).astype(bf16)

    own.wait()
    for offset in range(-(steps - 1), steps + 1):
        for q in range(PIECES):
            from_core(offset, q)

    owned = positions // n_tp
    width = w_ref.shape[1]
    quarter = n // 4

    def share(rows, group):
        left = both[rows, :]
        for slot in range(group * quarter, (group + 1) * quarter, 2):
            right = jnp.concatenate([weights[slot], weights[slot + 1]], axis=1)
            yield slot, jnp.dot(left, right, preferred_element_type=f32).astype(bf16)

    def out_copy(turn, group):
        cols = pl.ds(group * quarter * width, quarter * width)
        return pltpu.make_async_remote_copy(
            src_ref=gone_out.at[turn - 1, :, cols],
            dst_ref=come_out.at[turn - 1, :, cols],
            send_sem=out_send.at[turn - 1, group],
            recv_sem=out_recv.at[turn - 1, group],
            device_id={"tp": (tp + turn) % n_tp},
        )

    for turn in range(1, n_tp):
        target = (tp + turn) % n_tp
        rows = pl.ds(pl.multiple_of(target * owned, owned), owned)
        for group in range(4):
            for slot, value in share(rows, group):
                gone_out[turn - 1, :, slot * width : (slot + 2) * width] = value
            copy = out_copy(turn, group)
            copy.start()
            sends.append(copy)
    rows = pl.ds(pl.multiple_of(tp * owned, owned), owned)
    for group in range(4):
        for slot, value in share(rows, group):
            mine[:, slot * width : (slot + 2) * width] = value.astype(f32)
    for turn in range(1, n_tp):
        for group in range(4):
            out_copy(turn, group).wait_recv()
        mine[...] += come_out[turn - 1].astype(f32)
    summed = mine[...]
    out_ref[...] = (
        summed
        * lax.rsqrt(jnp.mean(summed * summed, axis=1, keepdims=True) + eps)
        * post_ref[...]
    ).astype(bf16)
    tail_copy.wait_send()
    for copy in sends:
        copy.wait_send()


def mix(proj, keep, extra, sgain, pool_mix, pgain, shard, post):
    n = lax.axis_size("sp")
    n_tp = lax.axis_size("tp")
    positions, heads = extra.shape
    head_cols = heads * DK
    depth, width = shard.shape
    steps = n // 4
    rounds = (n - 1).bit_length()
    owned = positions // n_tp
    model = n * width
    padded = -(-heads // 8) * 8
    f32, bf16, dma = jnp.float32, jnp.bfloat16, pltpu.SemaphoreType.DMA
    return pl.pallas_call(
        functools.partial(mix_kernel, n, n_tp),
        out_shape=jax.ShapeDtypeStruct((owned, model), bf16),
        in_specs=[pl.BlockSpec(memory_space=pltpu.VMEM)] * 8,
        out_specs=pl.BlockSpec(memory_space=pltpu.VMEM),
        scratch_shapes=[
            pltpu.VMEM((n, depth, width), bf16),
            pltpu.VMEM((positions, head_cols), f32),
            pltpu.VMEM((positions, head_cols), bf16),
            pltpu.VMEM((positions, 2 * head_cols), bf16),
            pltpu.VMEM((heads, DK, DK), f32),
            pltpu.VMEM((heads, DK, DK), f32),
            pltpu.VMEM((rounds, heads, DK, DK), bf16),
            pltpu.VMEM((rounds, padded, DK), f32),
            pltpu.VMEM((rounds, heads, DK, DK), bf16),
            pltpu.VMEM((rounds, padded, DK), f32),
            pltpu.VMEM((16, head_cols), bf16),
            pltpu.VMEM((16, head_cols), bf16),
            pltpu.VMEM((owned, model), f32),
            pltpu.VMEM((n_tp, owned, model), bf16),
            pltpu.VMEM((n_tp, owned, model), bf16),
            dma((2, steps, PIECES)),
            dma((2, steps, PIECES)),
            dma((2 * steps, PIECES)),
            dma((2 * steps, PIECES)),
            dma((rounds, 2)),
            dma((rounds, 2)),
            dma((2,)),
            dma,
            dma((n_tp, 4)),
            dma((n_tp, 4)),
        ],
        compiler_params=pltpu.CompilerParams(
            collective_id=1, has_side_effects=True, vmem_limit_bytes=56 * 1024 * 1024
        ),
        cost_estimate=pl.CostEstimate(
            flops=2 * positions * depth * model, bytes_accessed=4 * depth * width, transcendentals=0
        ),
    )(proj, keep, extra, sgain, pool_mix, pgain, shard, post)


def per_device(
    tokens_in,
    norm_gain,
    w_query,
    w_forget,
    w_input,
    w_rgate,
    w_pool_in,
    w_pgate,
    floor_rate,
    extra_logdecay,
    state_gain,
    pool_mix,
    pool_gain,
    out_rec,
    out_pool,
    post_gain,
):
    shard = jnp.concatenate(
        [w_query, w_forget, w_input, w_rgate, w_pool_in, w_pgate], axis=1
    )
    proj = project(tokens_in, norm_gain, shard)
    return mix(
        proj,
        -jnp.expm1(-floor_rate)[None, :],
        extra_logdecay,
        state_gain[None, :],
        pool_mix,
        pool_gain[None, :],
        jnp.concatenate([out_rec, out_pool], axis=0),
        post_gain[None, :],
    )


def solution(mesh):
    placed = (
        P("sp", "tp"),
        P(),
        P("sp", "tp"),
        P("sp", "tp"),
        P("sp", "tp"),
        P("sp", "tp"),
        P("sp", "tp"),
        P("sp", "tp"),
        P("tp"),
        P("sp", "tp"),
        P("tp"),
        P("tp", None, None),
        P("tp"),
        P("tp", "sp"),
        P("tp", "sp"),
        P(),
    )
    return jax.shard_map(
        per_device, mesh=mesh, in_specs=placed, out_specs=P(("sp", "tp"), None), check_vma=False
    )
```
